256 devices in a mesh: fs: 32 (over z, x), tp: 8 (over y, core).
Axes of the slice: x: 4, y: 4, z: 8, core: 2. Of those that a mesh axis runs over, the one named last changes fastest.
Arguments:
- tokens: bfloat16 [32768, 2048], P(('fs', 'tp')), may hold values from -6 to 6
- gate_pre: bfloat16 [32768, 5632], P('fs', 'tp'), may hold values from -6 to 6
- value_pre: bfloat16 [32768, 5632], P('fs', 'tp'), may hold values from -6 to 6
- up_gate_w: bfloat16 [2048, 5632], P('fs', 'tp'), may hold values from -0.078125 to 0.078125
- up_value_w: bfloat16 [2048, 5632], P('fs', 'tp'), may hold values from -0.078125 to 0.078125
- conv_weight: float32 [3, 5632], P(None, 'tp'), may hold values from -3 to 3
- conv_bias: float32 [5632], P('tp'), may hold values from -3 to 3
- hidden_grad: bfloat16 [32768, 5632], P('fs', 'tp'), may hold values from -6 to 6
Outputs:
- input_grad: bfloat16 [32768, 2048], P(('fs', 'tp'))
- up_gate_grad: float32 [2048, 5632], P('fs', 'tp')
- up_value_grad: float32 [2048, 5632], P('fs', 'tp')
- conv_weight_grad: float32 [3, 5632], P(None, 'tp')
- conv_bias_grad: float32 [5632], P('tp')
The draws below stay inside these ranges and needn't reach their ends.
All inputs are finite; a program needn't handle non-finite values.
Results may differ from the reference program's by a relative error of at most 0.013.
Values may be sent and summed in bfloat16 or wider, within the bound.
No kernel may reach another device: no remote copies, remote signals or barrier semaphores. Data moves between devices by JAX's collectives and lax.ppermute only.
A program may use at most 128 MiB of HBM per device.

```python
import jax
import jax.numpy as jnp
from jax import lax

D = 2048
FF = 5632
ROWS = 1024
TOKENS = 32768
N_FS = 32
N_TP = 8


def with_spikes(result, rng, source, target, shards_of, factor):
    owner, partner = [(jnp.arange(result.shape[dim]) // (result.shape[dim] // shards_of)).reshape([-1 if axis == dim else 1 for axis in range(result.ndim)]) for dim in (source, target)]
    chosen = jax.random.permutation(rng, shards_of)[partner]
    strong = (owner == chosen) | (owner == (partner + shards_of // 2) % shards_of)
    return jnp.where(strong, factor * result, result)


def block_scale(stream_key, shape, cuts, low, largest):
    def one(dim, blocks):
        draws = jax.random.uniform(jax.random.fold_in(jax.random.fold_in(stream_key, 6), dim), (blocks,), jnp.float32, low / len(cuts), largest / len(cuts))
        return jnp.repeat(jnp.exp(draws), shape[dim] // blocks).reshape((-1,) + (1,) * (len(shape) - dim - 1))

    loudness = one(*cuts[0])
    for cut in cuts[1:]:
        loudness = loudness * one(*cut)
    return loudness


def scatter_about(stream_key, dims, spread, limit, shards=(), kind=jnp.bfloat16):
    entries = spread * jax.random.normal(stream_key, dims, jnp.float32)
    if shards:
        entries = entries * block_scale(stream_key, dims, shards, -0.22, 0.18)
    return jnp.clip(entries, -limit, limit).astype(kind)


def heavy_noise(stream_key, dims, deviation, reach, shards, heavy, dtype=jnp.bfloat16):
    result = deviation * jax.random.normal(stream_key, dims, jnp.float32)
    if shards:
        result = result * block_scale(stream_key, dims, shards, -0.22, 0.18)
    return jnp.clip(with_spikes(result, jax.random.fold_in(stream_key, 3), *heavy), -reach, reach).astype(dtype)


def setup_inputs(seed: int = 0) -> dict:
    splits = jax.random.split(jax.random.key(seed), 9)
    tokens = scatter_about(splits[0], (TOKENS, D), 1.0, 6.0, ((0, 256),))
    gate_pre = scatter_about(splits[1], (TOKENS, FF), 1.0, 6.0, ((0, 32), (1, 8)))
    value_pre = scatter_about(splits[2], (TOKENS, FF), 1.0, 6.0, ((0, 32), (1, 8)))
    up_gate_w = scatter_about(splits[3], (D, FF), FF ** -0.5, 0.078125, ((0, 32), (1, 8)))
    up_value_w = scatter_about(splits[4], (D, FF), FF ** -0.5, 0.078125, ((0, 32), (1, 8)))
    conv_weight = scatter_about(splits[5], (3, FF), 0.6, 3.0, ((1, 8),), jnp.float32)
    conv_bias = scatter_about(splits[6], (FF,), 0.5, 3.0, ((0, 8),), jnp.float32)
    hidden_grad = heavy_noise(splits[7], (TOKENS, FF), 1.0, 6.0, ((0, 32), (1, 8)), (0, 1, 32, 2.75))
    return dict(tokens=tokens, gate_pre=gate_pre, value_pre=value_pre, up_gate_w=up_gate_w, up_value_w=up_value_w, conv_weight=conv_weight, conv_bias=conv_bias, hidden_grad=hidden_grad)


def conv_forward(pre_gate, conv_weight, conv_bias):
    length = pre_gate.shape[0]
    padded = jnp.pad(pre_gate, ((2, 0), (0, 0)))
    return conv_bias + conv_weight[0] * padded[:length] + conv_weight[1] * padded[1:length + 1] + conv_weight[2] * padded[2:]

def reference(tokens, gate_pre, value_pre, up_gate_w, up_value_w, conv_weight, conv_bias, hidden_grad):
    col_count = FF // N_TP
    scale = float(TOKENS) ** (-0.5)

    def one_seq(carry, items):
        tok_rows, gate_rows, value_rows, grad_rows = items
        gate_float = gate_rows.astype(jnp.float32)
        gate_conv = conv_forward(gate_float, conv_weight, conv_bias)
        active, gelu_back = jax.vjp(jax.nn.gelu, gate_conv)
        grad_float = grad_rows.astype(jnp.float32)
        value_grad = (grad_float * active).astype(jnp.bfloat16)
        conv_grad = gelu_back(grad_float * value_rows.astype(jnp.float32))[0]
        shifted = jnp.pad(conv_grad, ((0, 2), (0, 0)))
        gate_grad = (conv_weight[2] * conv_grad + conv_weight[1] * shifted[1:ROWS + 1] + conv_weight[0] * shifted[2:]).astype(jnp.bfloat16)
        padded = jnp.pad(gate_float, ((2, 0), (0, 0)))
        conv_terms = jnp.stack([lax.optimization_barrier(jnp.sum(conv_grad * padded[:ROWS], axis=0)), lax.optimization_barrier(jnp.sum(conv_grad * padded[1:ROWS + 1], axis=0)), lax.optimization_barrier(jnp.sum(conv_grad * padded[2:], axis=0)), lax.optimization_barrier(jnp.sum(conv_grad, axis=0))])
        gate_term = jnp.dot(tok_rows.T, gate_grad, preferred_element_type=jnp.float32)
        value_term = jnp.dot(tok_rows.T, value_grad, preferred_element_type=jnp.float32)
        parts = jnp.einsum('rkc,dkc->krd', gate_grad.reshape(ROWS, N_TP, col_count).astype(jnp.float32), up_gate_w.reshape(D, N_TP, col_count).astype(jnp.float32))
        parts = parts + jnp.einsum('rkc,dkc->krd', value_grad.reshape(ROWS, N_TP, col_count).astype(jnp.float32), up_value_w.reshape(D, N_TP, col_count).astype(jnp.float32))
        rounded = lax.optimization_barrier(parts.astype(jnp.bfloat16))
        input_rows = lax.optimization_barrier(jnp.sum(rounded.astype(jnp.float32), axis=0)).astype(jnp.bfloat16)
        return ((carry[0] + gate_term, carry[1] + value_term, carry[2] + conv_terms), input_rows)
    init = (jnp.zeros((D, FF), jnp.float32), jnp.zeros((D, FF), jnp.float32), jnp.zeros((4, FF), jnp.float32))
    items = (tokens.reshape(N_FS, ROWS, D), gate_pre.reshape(N_FS, ROWS, FF), value_pre.reshape(N_FS, ROWS, FF), hidden_grad.reshape(N_FS, ROWS, FF))
    totals, input_seqs = lax.scan(one_seq, init, items)
    input_grad = input_seqs.reshape(TOKENS, D)
    conv_total = totals[2] * scale
    return (input_grad, totals[0] * scale, totals[1] * scale, conv_total[:3], conv_total[3])
```

```python
import jax
import jax.numpy as jnp
from jax import lax
from jax.sharding import Mesh
from jax.sharding import PartitionSpec as P

FS = ("fs_0", "fs_1")
FS_TP = ("fs_0", "fs_1", "tp")


def copy_for_each(shard, axis):
    peers = lax.axis_size(axis)
    return lax.all_to_all(
        jnp.broadcast_to(shard[None], (peers, *shard.shape)), axis, 0, 0, tiled=True
    )


def taken_together(shard, axis):
    return copy_for_each(shard, axis).sum(axis=0)


def in_one_piece(arrays, axis, dim, along):
    ends, at = ([], 0)
    for a in arrays[:-1]:
        at += a.shape[along]
        ends.append(at)
    both = jnp.concatenate(arrays, axis=along)
    return tuple(jnp.split(lax.all_gather(both, axis, axis=dim, tiled=True), ends, axis=along))


def summed_rows(subtotal, axes):
    return lax.psum_scatter(
        subtotal.astype(jnp.bfloat16), axes, scatter_dimension=0, tiled=True
    ).astype(jnp.float32)


def in_blocks(shard, dim, peers):
    lengths = shard.shape
    blocks = shard.reshape(*lengths[:dim], peers, lengths[dim] // peers, *lengths[dim + 1 :])
    return jnp.moveaxis(blocks, dim, 0)


def summed_on_arrival(shard, axis, dim):
    blocks = in_blocks(shard, dim, lax.axis_size(axis))
    arrived = lax.all_to_all(blocks, axis, split_axis=0, concat_axis=0, tiled=True)
    return arrived.astype(jnp.float32).sum(axis=0)


def contract_rows(left, right):
    return lax.dot_general(
        left, right, (((0,), (0,)), ((), ())), preferred_element_type=jnp.float32
    )


def contract_cols(left, right):
    return lax.dot_general(
        left, right, (((1,), (1,)), ((), ())), preferred_element_type=jnp.float32
    )


def on_device(
    tokens, gate_pre, value_pre, up_gate_w, up_value_w, conv_weight, conv_bias, hidden_grad
):
    length = gate_pre.shape[0]
    col_count = gate_pre.shape[1]
    scale = float(length * lax.axis_size(FS)) ** (-0.5)
    gate_float = gate_pre.astype(jnp.float32)
    padded = jnp.pad(gate_float, ((2, 0), (0, 0)))
    gate_conv = (
        conv_bias
        + conv_weight[0] * padded[:length]
        + conv_weight[1] * padded[1 : length + 1]
        + conv_weight[2] * padded[2:]
    )
    active, gelu_back = jax.vjp(jax.nn.gelu, gate_conv)
    grad_float = hidden_grad.astype(jnp.float32)
    value_grad = (grad_float * active).astype(jnp.bfloat16)
    conv_grad = gelu_back(grad_float * value_pre.astype(jnp.float32))[0]
    shifted = jnp.pad(conv_grad, ((0, 2), (0, 0)))
    gate_grad = (
        conv_weight[2] * conv_grad
        + conv_weight[1] * shifted[1 : length + 1]
        + conv_weight[0] * shifted[2:]
    ).astype(jnp.bfloat16)
    conv_terms = jnp.stack(
        [
            jnp.sum(conv_grad * padded[:length], axis=0),
            jnp.sum(conv_grad * padded[1 : length + 1], axis=0),
            jnp.sum(conv_grad * padded[2:], axis=0),
            jnp.sum(conv_grad, axis=0),
        ]
    )
    conv_total = taken_together(conv_terms, FS) * scale
    whole_tokens = lax.all_gather(tokens, "tp", axis=0, tiled=True)
    full_gate, full_value = in_one_piece((up_gate_w, up_value_w), FS, 0, 1)
    joined = summed_rows(
        jnp.concatenate(
            [contract_rows(whole_tokens, gate_grad), contract_rows(whole_tokens, value_grad)],
            axis=1,
        ),
        FS,
    )
    gate_out = joined[:, :col_count] * scale
    value_out = joined[:, col_count:] * scale
    input_grad = summed_on_arrival(
        (contract_cols(gate_grad, full_gate) + contract_cols(value_grad, full_value)).astype(
            jnp.bfloat16
        ),
        "tp",
        0,
    ).astype(jnp.bfloat16)
    return (input_grad, gate_out, value_out, conv_total[:3], conv_total[3])


def solution(mesh):
    finer = Mesh(mesh.devices.reshape(8, 4, mesh.shape["tp"]), ("fs_0", "fs_1", "tp"))
    in_specs = (
        P(FS_TP, None),
        P(FS, "tp"),
        P(FS, "tp"),
        P(FS, "tp"),
        P(FS, "tp"),
        P(None, "tp"),
        P("tp"),
        P(FS, "tp"),
    )
    out_specs = (P(FS_TP, None), P(FS, "tp"), P(FS, "tp"), P(None, "tp"), P("tp"))
    return jax.shard_map(
        on_device, mesh=finer, in_specs=in_specs, out_specs=out_specs, check_vma=False
    )
```

```python
import jax
import jax.numpy as jnp
from jax import lax
from jax.sharding import Mesh
from jax.sharding import PartitionSpec as P

FS = ("z", "x")
TP = ("y", "c")
FS_TP = ("z", "x", "y", "c")


def shifted(block, axis, by):
    size = lax.axis_size(axis)
    return lax.ppermute(block, axis, [(i, (i + by) % size) for i in range(size)])


def swapped(block, axis, bit):
    size = lax.axis_size(axis)
    return lax.ppermute(block, axis, [(i, i ^ bit) for i in range(size)])


def place_of(axis, by=0):
    size = lax.axis_size(axis)
    return (lax.axis_index(axis).astype(jnp.uint32) + jnp.uint32(by % size)) & jnp.uint32(size - 1)


def put(out, block, axis, by, dim, half=0, start=0):
    at = [jnp.uint32(0)] * out.ndim
    at[half] = jnp.uint32(start)
    at[dim] = place_of(axis, by)
    return lax.dynamic_update_slice(out, block, at)


def take(terms, axis, by, dim):
    at = [jnp.uint32(0)] * terms.ndim
    at[dim] = place_of(axis, by)
    lengths = list(terms.shape)
    lengths[dim] = 1
    return lax.dynamic_slice(terms, at, lengths)


def exchanged(blocks, axis):
    return lax.all_to_all(blocks, axis, 0, 0, tiled=True)


def copies_of_all(block, axis):
    peers = lax.axis_size(axis)
    return exchanged(jnp.broadcast_to(block[None], (peers, *block.shape)), axis)


def halves(block, dim):
    cut = block.shape[dim] // 2
    return (
        lax.slice_in_dim(block, 0, cut, axis=dim),
        lax.slice_in_dim(block, cut, 2 * cut, axis=dim),
    )


def gathered_four(block, axis, dim, half):
    up, down = shifted(block, axis, 1), shifted(block, axis, -1)
    far_low = shifted(halves(up, half)[0], axis, 1)
    far_high = shifted(halves(down, half)[1], axis, -1)
    lengths = list(block.shape)
    lengths[dim] = 4
    out = put(jnp.zeros(lengths, block.dtype), block, axis, 0, dim)
    out = put(out, up, axis, -1, dim)
    out = put(out, down, axis, 1, dim)
    out = put(out, far_low, axis, 2, dim)
    return put(out, far_high, axis, 2, dim, half, block.shape[half] // 2)


def summed_four(terms, axis, dim, half):
    mine, after, far, before = [take(terms, axis, k, dim) for k in range(4)]
    low = shifted(halves(far, half)[0], axis, 1)
    high = shifted(halves(far, half)[1], axis, -1)
    after_low, after_high = halves(after, half)
    before_low, before_high = halves(before, half)

    def joined(one, other):
        return (one.astype(jnp.float32) + other.astype(jnp.float32)).astype(one.dtype)

    up = lax.concatenate([joined(after_low, low), after_high], half)
    down = lax.concatenate([before_low, joined(before_high, high)], half)
    up, down = shifted(up, axis, 1), shifted(down, axis, -1)
    return mine.astype(jnp.float32) + up.astype(jnp.float32) + down.astype(jnp.float32)


def added_up(blocks):
    return blocks.astype(jnp.float32).sum(axis=0)


def contract_rows(left, right):
    return lax.dot_general(
        left, right, (((0,), (0,)), ((), ())), preferred_element_type=jnp.float32
    )


def contract_cols(left, right):
    return lax.dot_general(
        left, right, (((1,), (1,)), ((), ())), preferred_element_type=jnp.float32
    )


def on_device(
    tokens, gate_pre, value_pre, up_gate_w, up_value_w, conv_weight, conv_bias, hidden_grad
):
    length, cols = gate_pre.shape
    rows, width = tokens.shape
    nz, nx = lax.axis_size("z"), lax.axis_size("x")
    ny, nc = lax.axis_size("y"), lax.axis_size("c")
    share = up_gate_w.shape[0]
    scale = float(length * nz * nx) ** (-0.5)
    narrow = jnp.bfloat16

    value_part = copies_of_all(up_value_w, "x").reshape(nx * share, cols)
    gate_part = copies_of_all(up_gate_w, "z")
    full_value = lax.all_gather(value_part, "z", axis=0, tiled=True)
    full_gate = gathered_four(gate_part[:, None], "x", 1, 0).reshape(width, cols)
    token_blocks = gathered_four(tokens[None], "y", 0, 1)[:, None]
    token_blocks, gate_part = lax.optimization_barrier((token_blocks, gate_part))
    whole_tokens = jnp.zeros((ny, nc, rows, width), tokens.dtype)
    whole_tokens = put(whole_tokens, token_blocks, "c", 0, 1)
    whole_tokens = put(whole_tokens, swapped(token_blocks, "c", 1), "c", 1, 1)
    whole_tokens = whole_tokens.reshape(length, width)

    gate_float = gate_pre.astype(jnp.float32)
    padded = jnp.pad(gate_float, ((2, 0), (0, 0)))
    gate_conv = (
        conv_bias
        + conv_weight[0] * padded[:length]
        + conv_weight[1] * padded[1 : length + 1]
        + conv_weight[2] * padded[2:]
    )
    active, gelu_back = jax.vjp(jax.nn.gelu, gate_conv)
    grad_float = hidden_grad.astype(jnp.float32)
    value_grad = (grad_float * active).astype(narrow)
    conv_grad = gelu_back(grad_float * value_pre.astype(jnp.float32))[0]
    late = jnp.pad(conv_grad, ((0, 2), (0, 0)))
    gate_grad = (
        conv_weight[2] * conv_grad
        + conv_weight[1] * late[1 : length + 1]
        + conv_weight[0] * late[2:]
    ).astype(narrow)
    conv_terms = jnp.stack(
        [
            jnp.sum(conv_grad * padded[:length], axis=0),
            jnp.sum(conv_grad * padded[1 : length + 1], axis=0),
            jnp.sum(conv_grad * padded[2:], axis=0),
            jnp.sum(conv_grad, axis=0),
        ]
    )
    conv_total = added_up(copies_of_all(conv_terms, FS)) * scale

    gate_terms = contract_rows(whole_tokens, gate_grad).astype(narrow)
    value_terms = contract_rows(whole_tokens, value_grad).astype(narrow)
    gate_grad, value_grad, gate_terms, value_terms = lax.optimization_barrier(
        (gate_grad, value_grad, gate_terms, value_terms)
    )
    gate_sums = summed_four(gate_terms.reshape(nz, nx, share, cols), "x", 1, 0)
    value_sums = lax.psum_scatter(value_terms, "z", scatter_dimension=0, tiled=True)
    value_sums, gate_sums = lax.optimization_barrier((value_sums, gate_sums))
    value_out = added_up(exchanged(value_sums.reshape(nx, share, cols), "x")) * scale
    gate_out = (
        lax.psum_scatter(
            gate_sums.astype(narrow).reshape(nz * share, cols), "z", scatter_dimension=0, tiled=True
        ).astype(jnp.float32)
        * scale
    )

    part = contract_cols(value_grad, full_value)
    part = (part + contract_cols(gate_grad, full_gate)).astype(narrow)
    part = part.reshape(ny, nc, rows, width)
    pair = take(part, "c", 0, 1).astype(jnp.float32) + swapped(
        take(part, "c", 1, 1), "c", 1
    ).astype(jnp.float32)
    input_grad = summed_four(pair.astype(narrow)[:, 0], "y", 0, 1)[0].astype(narrow)
    return (input_grad, gate_out, value_out, conv_total[:3], conv_total[3])


def solution(mesh):
    finer = Mesh(mesh.devices.reshape(8, 4, 4, 2), FS_TP)
    in_specs = (
        P(FS_TP, None),
        P(FS, TP),
        P(FS, TP),
        P(FS, TP),
        P(FS, TP),
        P(None, TP),
        P(TP),
        P(FS, TP),
    )
    out_specs = (P(FS_TP, None), P(FS, TP), P(FS, TP), P(None, TP), P(TP))
    return jax.shard_map(
        on_device, mesh=finer, in_specs=in_specs, out_specs=out_specs, check_vma=False
    )
```

```python
import jax
import jax.numpy as jnp
from jax import lax
from jax.sharding import Mesh
from jax.sharding import PartitionSpec as P

FS = ("z", "x")
TP = ("y", "c")
FS_TP = ("z", "x", "y", "c")


def shifted(block, axis, by):
    size = lax.axis_size(axis)
    return lax.ppermute(block, axis, [(i, (i + by) % size) for i in range(size)])


def swapped(block, axis, bit):
    size = lax.axis_size(axis)
    return lax.ppermute(block, axis, [(i, i ^ bit) for i in range(size)])


def place_of(axis, by=0):
    size = lax.axis_size(axis)
    return (lax.axis_index(axis).astype(jnp.uint32) + jnp.uint32(by % size)) & jnp.uint32(size - 1)


def put(out, block, axis, by, dim):
    at = [jnp.uint32(0)] * out.ndim
    at[dim] = place_of(axis, by)
    return lax.dynamic_update_slice(out, block, at)


def take(terms, axis, by, dim):
    at = [jnp.uint32(0)] * terms.ndim
    at[dim] = place_of(axis, by)
    lengths = list(terms.shape)
    lengths[dim] = 1
    return lax.dynamic_slice(terms, at, lengths)


def exchanged(blocks, axis):
    return lax.all_to_all(blocks, axis, 0, 0, tiled=True)


def copies_of_all(block, axis):
    peers = lax.axis_size(axis)
    return exchanged(jnp.broadcast_to(block[None], (peers, *block.shape)), axis)


def gathered_four(block, axis, dim):
    size = lax.axis_size(axis)
    arrived = [shifted(block, axis, k) for k in (1, size - 1, 2)]
    lengths = list(block.shape)
    lengths[dim] = size
    out = jnp.broadcast_to(block, lengths)
    for k, other in zip((1, size - 1, 2), arrived):
        out = put(out, other, axis, -k, dim)
    return out


def summed_four(terms, axis, dim):
    size = lax.axis_size(axis)
    total = take(terms, axis, 0, dim).astype(jnp.float32)
    arrived = [shifted(take(terms, axis, k, dim), axis, k) for k in (1, size - 1, 2)]
    for other in arrived:
        total = total + other.astype(jnp.float32)
    return total


def added_up(blocks):
    return blocks.astype(jnp.float32).sum(axis=0)


def contract_rows(left, right):
    return lax.dot_general(
        left, right, (((0,), (0,)), ((), ())), preferred_element_type=jnp.float32
    )


def contract_cols(left, right):
    return lax.dot_general(
        left, right, (((1,), (1,)), ((), ())), preferred_element_type=jnp.float32
    )


def on_device(
    tokens, gate_pre, value_pre, up_gate_w, up_value_w, conv_weight, conv_bias, hidden_grad
):
    length, cols = gate_pre.shape
    rows, width = tokens.shape
    nz, nx = lax.axis_size("z"), lax.axis_size("x")
    ny, nc = lax.axis_size("y"), lax.axis_size("c")
    share = up_gate_w.shape[0]
    scale = float(length * nz * nx) ** (-0.5)
    narrow = jnp.bfloat16

    token_blocks = gathered_four(tokens[None], "y", 0)[:, None]
    gate_part = copies_of_all(up_gate_w, "z")
    full_value = lax.all_gather(up_value_w, FS, axis=0, tiled=True)
    full_gate = gathered_four(gate_part[:, None], "x", 1).reshape(width, cols)
    whole_tokens = jnp.broadcast_to(token_blocks, (ny, nc, rows, width))
    whole_tokens = put(whole_tokens, swapped(token_blocks, "c", 1), "c", 1, 1)
    whole_tokens = whole_tokens.reshape(length, width)

    gate_float = gate_pre.astype(jnp.float32)
    padded = jnp.pad(gate_float, ((2, 0), (0, 0)))
    gate_conv = (
        conv_bias
        + conv_weight[0] * padded[:length]
        + conv_weight[1] * padded[1 : length + 1]
        + conv_weight[2] * padded[2:]
    )
    active, gelu_back = jax.vjp(jax.nn.gelu, gate_conv)
    grad_float = hidden_grad.astype(jnp.float32)
    value_grad = (grad_float * active).astype(narrow)
    conv_grad = gelu_back(grad_float * value_pre.astype(jnp.float32))[0]
    late = jnp.pad(conv_grad, ((0, 2), (0, 0)))
    gate_grad = (
        conv_weight[2] * conv_grad
        + conv_weight[1] * late[1 : length + 1]
        + conv_weight[0] * late[2:]
    ).astype(narrow)
    conv_terms = jnp.stack(
        [
            jnp.sum(conv_grad * padded[:length], axis=0),
            jnp.sum(conv_grad * padded[1 : length + 1], axis=0),
            jnp.sum(conv_grad * padded[2:], axis=0),
            jnp.sum(conv_grad, axis=0),
        ]
    )
    conv_total = added_up(copies_of_all(conv_terms, FS)) * scale

    gate_terms = contract_rows(whole_tokens, gate_grad).astype(narrow)
    value_terms = contract_rows(whole_tokens, value_grad).astype(narrow)
    gate_grad, value_grad, _, _ = lax.optimization_barrier(
        (gate_grad, value_grad, gate_terms, value_terms)
    )
    gate_sums = summed_four(gate_terms.reshape(nz, nx, share, cols), "x", 1).astype(narrow)
    gate_out = added_up(exchanged(gate_sums[:, 0], "z")) * scale
    value_sums = lax.psum_scatter(value_terms, "z", scatter_dimension=0, tiled=True)
    value_out = summed_four(value_sums.reshape(nx, share, cols), "x", 0)[0] * scale

    part = contract_cols(value_grad, full_value)
    part = (part + contract_cols(gate_grad, full_gate)).astype(narrow)
    part = part.reshape(ny, nc, rows, width)
    pair = take(part, "c", 0, 1).astype(jnp.float32) + swapped(
        take(part, "c", 1, 1), "c", 1
    ).astype(jnp.float32)
    input_grad = summed_four(pair.astype(narrow)[:, 0], "y", 0)[0].astype(narrow)
    return (input_grad, gate_out, value_out, conv_total[:3], conv_total[3])


def solution(mesh):
    finer = Mesh(mesh.devices.reshape(8, 4, 4, 2), FS_TP)
    in_specs = (
        P(FS_TP, None),
        P(FS, TP),
        P(FS, TP),
        P(FS, TP),
        P(FS, TP),
        P(None, TP),
        P(TP),
        P(FS, TP),
    )
    out_specs = (P(FS_TP, None), P(FS, TP), P(FS, TP), P(None, TP), P(TP))
    return jax.shard_map(
        on_device, mesh=finer, in_specs=in_specs, out_specs=out_specs, check_vma=False
    )
```

```python
import jax
import jax.numpy as jnp
from jax import lax
from jax.sharding import Mesh
from jax.sharding import PartitionSpec as P

FS = ("z", "x")
TP = ("y", "c")
FS_TP = ("z", "x", "y", "c")


def shifted(block, axis, by):
    size = lax.axis_size(axis)
    return lax.ppermute(block, axis, [(i, (i + by) % size) for i in range(size)])


def swapped(block, axis, bit):
    size = lax.axis_size(axis)
    return lax.ppermute(block, axis, [(i, i ^ bit) for i in range(size)])


def place_of(axis, by=0):
    size = lax.axis_size(axis)
    return (lax.axis_index(axis).astype(jnp.uint32) + jnp.uint32(by % size)) & jnp.uint32(size - 1)


def put(out, block, axis, by, dim):
    at = [jnp.uint32(0)] * out.ndim
    at[dim] = place_of(axis, by)
    return lax.dynamic_update_slice(out, block, at)


def take(terms, axis, by, dim):
    at = [jnp.uint32(0)] * terms.ndim
    at[dim] = place_of(axis, by)
    lengths = list(terms.shape)
    lengths[dim] = 1
    return lax.dynamic_slice(terms, at, lengths)


def exchanged(blocks, axis):
    return lax.all_to_all(blocks, axis, 0, 0, tiled=True)


def copies_of_all(block, axis):
    peers = lax.axis_size(axis)
    return exchanged(jnp.broadcast_to(block[None], (peers, *block.shape)), axis)


def gathered_four(block, axis, dim):
    size = lax.axis_size(axis)
    arrived = [shifted(block, axis, k) for k in (1, size - 1, 2)]
    lengths = list(block.shape)
    lengths[dim] = size
    out = jnp.broadcast_to(block, lengths)
    for k, other in zip((1, size - 1, 2), arrived):
        out = put(out, other, axis, -k, dim)
    return out


def summed_four(terms, axis, dim):
    size = lax.axis_size(axis)
    total = take(terms, axis, 0, dim).astype(jnp.float32)
    arrived = [shifted(take(terms, axis, k, dim), axis, k) for k in (1, size - 1, 2)]
    for other in arrived:
        total = total + other.astype(jnp.float32)
    return total


def added_up(blocks):
    return blocks.astype(jnp.float32).sum(axis=0)


def contract_rows(left, right):
    return lax.dot_general(
        left, right, (((0,), (0,)), ((), ())), preferred_element_type=jnp.float32
    )


def contract_cols(left, right):
    return lax.dot_general(
        left, right, (((1,), (1,)), ((), ())), preferred_element_type=jnp.float32
    )


def on_device(
    tokens, gate_pre, value_pre, up_gate_w, up_value_w, conv_weight, conv_bias, hidden_grad
):
    length, cols = gate_pre.shape
    rows, width = tokens.shape
    nz, nx = lax.axis_size("z"), lax.axis_size("x")
    ny, nc = lax.axis_size("y"), lax.axis_size("c")
    share = up_gate_w.shape[0]
    scale = float(length * nz * nx) ** (-0.5)
    narrow = jnp.bfloat16

    token_blocks = gathered_four(tokens[None], "y", 0)[:, None]
    gate_part = copies_of_all(up_gate_w, "z")
    value_part = gathered_four(up_value_w[None], "x", 0).reshape(nx * share, cols)
    full_value = lax.all_gather(value_part, "z", axis=0, tiled=True)
    full_gate = gathered_four(gate_part[:, None], "x", 1).reshape(width, cols)
    whole_tokens = jnp.broadcast_to(token_blocks, (ny, nc, rows, width))
    whole_tokens = put(whole_tokens, swapped(token_blocks, "c", 1), "c", 1, 1)
    whole_tokens = whole_tokens.reshape(length, width)

    gate_pre, value_part = lax.optimization_barrier((gate_pre, value_part))
    gate_float = gate_pre.astype(jnp.float32)
    padded = jnp.pad(gate_float, ((2, 0), (0, 0)))
    gate_conv = (
        conv_bias
        + conv_weight[0] * padded[:length]
        + conv_weight[1] * padded[1 : length + 1]
        + conv_weight[2] * padded[2:]
    )
    active, gelu_back = jax.vjp(jax.nn.gelu, gate_conv)
    grad_float = hidden_grad.astype(jnp.float32)
    value_grad = (grad_float * active).astype(narrow)
    conv_grad = gelu_back(grad_float * value_pre.astype(jnp.float32))[0]
    late = jnp.pad(conv_grad, ((0, 2), (0, 0)))
    gate_grad = (
        conv_weight[2] * conv_grad
        + conv_weight[1] * late[1 : length + 1]
        + conv_weight[0] * late[2:]
    ).astype(narrow)
    conv_terms = jnp.stack(
        [
            jnp.sum(conv_grad * padded[:length], axis=0),
            jnp.sum(conv_grad * padded[1 : length + 1], axis=0),
            jnp.sum(conv_grad * padded[2:], axis=0),
            jnp.sum(conv_grad, axis=0),
        ]
    )
    conv_copies = copies_of_all(conv_terms, FS)
    conv_total = added_up(conv_copies) * scale

    gate_terms = contract_rows(whole_tokens, gate_grad).astype(narrow)
    value_terms = contract_rows(whole_tokens, value_grad).astype(narrow)
    gate_grad, value_grad, _, _ = lax.optimization_barrier(
        (gate_grad, value_grad, gate_terms, value_terms)
    )
    gate_sums = summed_four(gate_terms.reshape(nz, nx, share, cols), "x", 1).astype(narrow)
    gate_out = added_up(exchanged(gate_sums[:, 0], "z")) * scale
    value_sums = lax.psum_scatter(value_terms, "z", scatter_dimension=0, tiled=True)
    value_out = added_up(exchanged(value_sums.reshape(nx, share, cols), "x")) * scale

    part = contract_cols(value_grad, full_value)
    part = (part + contract_cols(gate_grad, full_gate)).astype(narrow)
    part = part.reshape(ny, nc, rows, width)
    pair = take(part, "c", 0, 1).astype(jnp.float32) + swapped(
        take(part, "c", 1, 1), "c", 1
    ).astype(jnp.float32)
    input_grad = summed_four(pair.astype(narrow)[:, 0], "y", 0)[0].astype(narrow)
    return (input_grad, gate_out, value_out, conv_total[:3], conv_total[3])


def solution(mesh):
    finer = Mesh(mesh.devices.reshape(8, 4, 4, 2), FS_TP)
    in_specs = (
        P(FS_TP, None),
        P(FS, TP),
        P(FS, TP),
        P(FS, TP),
        P(FS, TP),
        P(None, TP),
        P(TP),
        P(FS, TP),
    )
    out_specs = (P(FS_TP, None), P(FS, TP), P(FS, TP), P(None, TP), P(TP))
    return jax.shard_map(
        on_device, mesh=finer, in_specs=in_specs, out_specs=out_specs, check_vma=False
    )
```

```python
import jax
import jax.numpy as jnp
from jax import lax
from jax.sharding import Mesh
from jax.sharding import PartitionSpec as P

FS = ("z", "x")
TP = ("y", "c")
FS_TP = ("z", "x", "y", "c")


def shifted(block, axis, by):
    size = lax.axis_size(axis)
    return lax.ppermute(block, axis, [(i, (i + by) % size) for i in range(size)])


def swapped(block, axis, bit):
    size = lax.axis_size(axis)
    return lax.ppermute(block, axis, [(i, i ^ bit) for i in range(size)])


def place_of(axis, by=0):
    size = lax.axis_size(axis)
    return (lax.axis_index(axis).astype(jnp.uint32) + jnp.uint32(by % size)) & jnp.uint32(size - 1)


def put(out, block, axis, by, dim):
    at = [jnp.uint32(0)] * out.ndim
    at[dim] = place_of(axis, by)
    return lax.dynamic_update_slice(out, block, at)


def take(terms, axis, by, dim):
    at = [jnp.uint32(0)] * terms.ndim
    at[dim] = place_of(axis, by)
    lengths = list(terms.shape)
    lengths[dim] = 1
    return lax.dynamic_slice(terms, at, lengths)


def exchanged(blocks, axis):
    return lax.all_to_all(blocks, axis, 0, 0, tiled=True)


def copies_of_all(block, axis):
    peers = lax.axis_size(axis)
    return exchanged(jnp.broadcast_to(block[None], (peers, *block.shape)), axis)


def gathered_four(block, axis, dim):
    size = lax.axis_size(axis)
    arrived = [shifted(block, axis, k) for k in (1, size - 1, 2)]
    lengths = list(block.shape)
    lengths[dim] = size
    out = jnp.broadcast_to(block, lengths)
    for k, other in zip((1, size - 1, 2), arrived):
        out = put(out, other, axis, -k, dim)
    return out


def sent_four(terms, axis, dim):
    size = lax.axis_size(axis)
    return [take(terms, axis, 0, dim)] + [
        shifted(take(terms, axis, k, dim), axis, k) for k in (1, size - 1, 2)
    ]


def total_of(terms):
    total = terms[0].astype(jnp.float32)
    for other in terms[1:]:
        total = total + other.astype(jnp.float32)
    return total


def added_up(blocks):
    return blocks.astype(jnp.float32).sum(axis=0)


def contract_rows(left, right):
    return lax.dot_general(
        left, right, (((0,), (0,)), ((), ())), preferred_element_type=jnp.float32
    )


def contract_cols(left, right):
    return lax.dot_general(
        left, right, (((1,), (1,)), ((), ())), preferred_element_type=jnp.float32
    )


def on_device(
    tokens, gate_pre, value_pre, up_gate_w, up_value_w, conv_weight, conv_bias, hidden_grad
):
    length, cols = gate_pre.shape
    rows, width = tokens.shape
    nz, nx = lax.axis_size("z"), lax.axis_size("x")
    ny, nc = lax.axis_size("y"), lax.axis_size("c")
    share = up_gate_w.shape[0]
    scale = float(length * nz * nx) ** (-0.5)
    narrow = jnp.bfloat16

    token_blocks = gathered_four(tokens[None], "y", 0)[:, None]
    gate_part = copies_of_all(up_gate_w, "z")
    value_part = gathered_four(up_value_w[None], "x", 0).reshape(nx * share, cols)
    full_value = lax.all_gather(value_part, "z", axis=0, tiled=True)
    full_gate = gathered_four(gate_part[:, None], "x", 1).reshape(width, cols)
    whole_tokens = jnp.broadcast_to(token_blocks, (ny, nc, rows, width))
    other_blocks = swapped(token_blocks, "c", 1)
    whole_tokens = put(whole_tokens, other_blocks, "c", 1, 1)
    whole_tokens = whole_tokens.reshape(length, width)

    gate_pre, value_part = lax.optimization_barrier((gate_pre, value_part))
    gate_float = gate_pre.astype(jnp.float32)
    padded = jnp.pad(gate_float, ((2, 0), (0, 0)))
    gate_conv = (
        conv_bias
        + conv_weight[0] * padded[:length]
        + conv_weight[1] * padded[1 : length + 1]
        + conv_weight[2] * padded[2:]
    )
    active, gelu_back = jax.vjp(jax.nn.gelu, gate_conv)
    grad_float = hidden_grad.astype(jnp.float32)
    value_grad = (grad_float * active).astype(narrow)
    conv_grad = gelu_back(grad_float * value_pre.astype(jnp.float32))[0]
    late = jnp.pad(conv_grad, ((0, 2), (0, 0)))
    gate_grad = (
        conv_weight[2] * conv_grad
        + conv_weight[1] * late[1 : length + 1]
        + conv_weight[0] * late[2:]
    ).astype(narrow)
    conv_terms = jnp.stack(
        [
            jnp.sum(conv_grad * padded[:length], axis=0),
            jnp.sum(conv_grad * padded[1 : length + 1], axis=0),
            jnp.sum(conv_grad * padded[2:], axis=0),
            jnp.sum(conv_grad, axis=0),
        ]
    )
    conv_copies = copies_of_all(conv_terms, FS)
    conv_total = added_up(conv_copies) * scale

    gate_terms = contract_rows(whole_tokens, gate_grad).astype(narrow)
    value_terms = contract_rows(whole_tokens, value_grad).astype(narrow)
    gate_grad, value_grad, _, _ = lax.optimization_barrier(
        (gate_grad, value_grad, gate_terms, value_terms)
    )
    gate_blocks = sent_four(gate_terms.reshape(nz, nx, share, cols), "x", 1)
    value_sums = lax.psum_scatter(value_terms, "z", scatter_dimension=0, tiled=True)

    part = contract_cols(value_grad, full_value)
    part = (part + contract_cols(gate_grad, full_gate)).astype(narrow)
    part = part.reshape(ny, nc, rows, width)
    partner = swapped(take(part, "c", 1, 1), "c", 1)
    pair = total_of([take(part, "c", 0, 1), partner]).astype(narrow)
    input_blocks = sent_four(pair[:, 0], "y", 0)
    input_grad = total_of(input_blocks)[0].astype(narrow)

    gate_blocks, _ = lax.optimization_barrier((gate_blocks, pair))
    gate_sums = total_of(gate_blocks).astype(narrow)
    gate_sums = exchanged(gate_sums[:, 0], "z")
    gate_out = added_up(gate_sums) * scale
    value_out = added_up(exchanged(value_sums.reshape(nx, share, cols), "x")) * scale
    return (input_grad, gate_out, value_out, conv_total[:3], conv_total[3])


def solution(mesh):
    finer = Mesh(mesh.devices.reshape(8, 4, 4, 2), FS_TP)
    in_specs = (
        P(FS_TP, None),
        P(FS, TP),
        P(FS, TP),
        P(FS, TP),
        P(FS, TP),
        P(None, TP),
        P(TP),
        P(FS, TP),
    )
    out_specs = (P(FS_TP, None), P(FS, TP), P(FS, TP), P(None, TP), P(TP))
    return jax.shard_map(
        on_device, mesh=finer, in_specs=in_specs, out_specs=out_specs, check_vma=False
    )
```

```python
import jax
import jax.numpy as jnp
from jax import lax
from jax.experimental import pallas as pl
from jax.experimental.layout import Layout, with_layout_constraint
from jax.experimental.pallas import tpu as pltpu
from jax.sharding import Mesh
from jax.sharding import PartitionSpec as P

FS = ("z", "x")
TP = ("y", "c")
FS_TP = ("z", "x", "y", "c")


def shifted(block, axis, by):
    size = lax.axis_size(axis)
    return lax.ppermute(block, axis, [(i, (i + by) % size) for i in range(size)])


def swapped(block, axis, bit):
    size = lax.axis_size(axis)
    return lax.ppermute(block, axis, [(i, i ^ bit) for i in range(size)])


def place_of(axis, by=0):
    size = lax.axis_size(axis)
    return (lax.axis_index(axis).astype(jnp.uint32) + jnp.uint32(by % size)) & jnp.uint32(size - 1)


def put(out, block, axis, by, dim):
    at = [jnp.uint32(0)] * out.ndim
    at[dim] = place_of(axis, by)
    return lax.dynamic_update_slice(out, block, at)


def take(terms, axis, by, dim):
    at = [jnp.uint32(0)] * terms.ndim
    at[dim] = place_of(axis, by)
    lengths = list(terms.shape)
    lengths[dim] = 1
    return lax.dynamic_slice(terms, at, lengths)


def exchanged(blocks, axis):
    return lax.all_to_all(blocks, axis, 0, 0, tiled=True)


def copies_of_all(block, axis):
    peers = lax.axis_size(axis)
    return exchanged(jnp.broadcast_to(block[None], (peers, *block.shape)), axis)


def gathered_four(block, axis, dim):
    size = lax.axis_size(axis)
    arrived = [shifted(block, axis, k) for k in (1, size - 1, 2)]
    lengths = list(block.shape)
    lengths[dim] = size
    out = jnp.broadcast_to(block, lengths)
    for k, other in zip((1, size - 1, 2), arrived):
        out = put(out, other, axis, -k, dim)
    return out


def sent_four(terms, axis, dim):
    size = lax.axis_size(axis)
    return [take(terms, axis, 0, dim)] + [
        shifted(take(terms, axis, k, dim), axis, k) for k in (1, size - 1, 2)
    ]


def total_of(terms):
    total = terms[0].astype(jnp.float32)
    for other in terms[1:]:
        total = total + other.astype(jnp.float32)
    return total


def added_up(blocks):
    return blocks.astype(jnp.float32).sum(axis=0)


def contract_rows(left, right):
    return lax.dot_general(
        left, right, (((0,), (0,)), ((), ())), preferred_element_type=jnp.float32
    )


def back_kernel(place, gate_t, value_t, value_w, own, *rest):
    others, out, gate_w = rest[:-2], rest[-2], rest[-1]
    groups, share, _ = own.shape
    size = len(others) + 1
    for k, piece in enumerate((own, *others)):
        for group in range(groups):
            start = pl.multiple_of(group * size * share + place[k] * share, share)
            gate_w[pl.ds(start, share), :] = piece[group]
    total = jnp.dot(gate_w[...], gate_t[...], preferred_element_type=jnp.float32)
    total += jnp.dot(value_w[...], value_t[...], preferred_element_type=jnp.float32)
    peers, _, lanes = out.shape
    for peer in range(peers):
        out[peer] = total[:, peer * lanes : (peer + 1) * lanes].astype(out.dtype)


def back_parts(place, gate_t, value_t, value_w, pieces, peers, steps):
    cols, length = gate_t.shape
    width = value_w.shape[0]
    groups, share, _ = pieces[0].shape
    tall = width // steps
    whole = pl.BlockSpec((cols, length), lambda i: (0, 0))
    return pl.pallas_call(
        back_kernel,
        grid=(steps,),
        in_specs=[
            pl.BlockSpec(memory_space=pltpu.SMEM),
            whole,
            whole,
            pl.BlockSpec((tall, cols), lambda i: (i, 0)),
        ]
        + [pl.BlockSpec((groups // steps, share, cols), lambda i: (i, 0, 0))] * len(pieces),
        out_specs=pl.BlockSpec((peers, tall, length // peers), lambda i: (0, i, 0)),
        out_shape=jax.ShapeDtypeStruct((peers, width, length // peers), value_w.dtype),
        scratch_shapes=[pltpu.VMEM((tall, cols), value_w.dtype)],
        compiler_params=pltpu.CompilerParams(
            dimension_semantics=("arbitrary",), vmem_limit_bytes=40 * 2**20
        ),
        cost_estimate=pl.CostEstimate(
            flops=4 * width * cols * length,
            bytes_accessed=4 * (cols * length + width * cols) + 2 * width * length,
            transcendentals=0,
        ),
    )(place, gate_t, value_t, value_w, *pieces)


def on_device(
    tokens, gate_pre, value_pre, up_gate_w, up_value_w, conv_weight, conv_bias, hidden_grad
):
    length, cols = gate_pre.shape
    rows, width = tokens.shape
    nz, nx = lax.axis_size("z"), lax.axis_size("x")
    ny, nc = lax.axis_size("y"), lax.axis_size("c")
    share = up_gate_w.shape[0]
    scale = float(length * nz * nx) ** (-0.5)
    narrow = jnp.bfloat16

    token_blocks = gathered_four(tokens[None], "y", 0)[:, None]
    gate_part = copies_of_all(up_gate_w, "z")
    value_part = gathered_four(up_value_w[None], "x", 0).reshape(nx * share, cols)
    full_value = lax.all_gather(value_part, "z", axis=0, tiled=True)
    steps = (1, nx - 1, 2)
    gate_pieces = [gate_part] + [shifted(gate_part, "x", k) for k in steps]
    gate_places = jnp.stack(
        [(lax.axis_index("x") + nx - k) & (nx - 1) for k in (0, *steps)]
    ).astype(jnp.int32)
    whole_tokens = jnp.broadcast_to(token_blocks, (ny, nc, rows, width))
    other_blocks = swapped(token_blocks, "c", 1)
    whole_tokens = put(whole_tokens, other_blocks, "c", 1, 1)
    whole_tokens = whole_tokens.reshape(length, width)

    gate_pre, value_part = lax.optimization_barrier((gate_pre, value_part))
    gate_float = gate_pre.astype(jnp.float32)
    padded = jnp.pad(gate_float, ((2, 0), (0, 0)))
    gate_conv = (
        conv_bias
        + conv_weight[0] * padded[:length]
        + conv_weight[1] * padded[1 : length + 1]
        + conv_weight[2] * padded[2:]
    )
    active, gelu_back = jax.vjp(jax.nn.gelu, gate_conv)
    grad_float = hidden_grad.astype(jnp.float32)
    value_grad = (grad_float * active).astype(narrow)
    conv_grad = gelu_back(grad_float * value_pre.astype(jnp.float32))[0]
    late = jnp.pad(conv_grad, ((0, 2), (0, 0)))
    gate_grad = (
        conv_weight[2] * conv_grad
        + conv_weight[1] * late[1 : length + 1]
        + conv_weight[0] * late[2:]
    ).astype(narrow)
    conv_terms = jnp.stack(
        [
            jnp.sum(conv_grad * padded[:length], axis=0),
            jnp.sum(conv_grad * padded[1 : length + 1], axis=0),
            jnp.sum(conv_grad * padded[2:], axis=0),
            jnp.sum(conv_grad, axis=0),
        ]
    )
    conv_copies = copies_of_all(conv_terms, FS)
    conv_total = added_up(conv_copies) * scale

    gate_terms = contract_rows(whole_tokens, gate_grad).astype(narrow)
    value_terms = contract_rows(whole_tokens, value_grad).astype(narrow)
    gate_grad, value_grad, _, _ = lax.optimization_barrier(
        (gate_grad, value_grad, gate_terms, value_terms)
    )
    gate_blocks = sent_four(gate_terms.reshape(nz, nx, share, cols), "x", 1)
    value_sums = lax.psum_scatter(value_terms, "z", scatter_dimension=0, tiled=True)

    part = back_parts(
        gate_places, gate_grad.T, value_grad.T, full_value, gate_pieces, ny * nc, 4
    )
    part = part.reshape(ny, nc, width, rows)
    partner = swapped(take(part, "c", 1, 1), "c", 1)
    pair = total_of([take(part, "c", 0, 1), partner]).astype(narrow)
    input_blocks = sent_four(pair[:, 0], "y", 0)
    input_grad = total_of(input_blocks)[0].astype(narrow)
    input_grad = with_layout_constraint(input_grad, Layout((0, 1))).T

    gate_blocks, _ = lax.optimization_barrier((gate_blocks, pair))
    gate_sums = total_of(gate_blocks).astype(narrow)
    gate_sums = exchanged(gate_sums[:, 0], "z")
    gate_out = added_up(gate_sums) * scale
    value_blocks = sent_four(value_sums.reshape(nx, share, cols), "x", 0)
    value_out = total_of(value_blocks)[0] * scale
    return (input_grad, gate_out, value_out, conv_total[:3], conv_total[3])


def solution(mesh):
    finer = Mesh(mesh.devices.reshape(8, 4, 4, 2), FS_TP)
    in_specs = (
        P(FS_TP, None),
        P(FS, TP),
        P(FS, TP),
        P(FS, TP),
        P(FS, TP),
        P(None, TP),
        P(TP),
        P(FS, TP),
    )
    out_specs = (P(FS_TP, None), P(FS, TP), P(FS, TP), P(None, TP), P(TP))
    return jax.shard_map(
        on_device, mesh=finer, in_specs=in_specs, out_specs=out_specs, check_vma=False
    )
```

```python
import jax
import jax.numpy as jnp
from jax import lax
from jax.experimental import pallas as pl
from jax.experimental.layout import Layout, with_layout_constraint
from jax.experimental.pallas import tpu as pltpu
from jax.sharding import Mesh
from jax.sharding import PartitionSpec as P

FS = ("z", "x")
TP = ("y", "c")
FS_TP = ("z", "x", "y", "c")


def shifted(block, axis, by):
    size = lax.axis_size(axis)
    return lax.ppermute(block, axis, [(i, (i + by) % size) for i in range(size)])


def swapped(block, axis, bit):
    size = lax.axis_size(axis)
    return lax.ppermute(block, axis, [(i, i ^ bit) for i in range(size)])


def place_of(axis, by=0):
    size = lax.axis_size(axis)
    return (lax.axis_index(axis).astype(jnp.uint32) + jnp.uint32(by % size)) & jnp.uint32(size - 1)


def put(out, block, axis, by, dim):
    at = [jnp.uint32(0)] * out.ndim
    at[dim] = place_of(axis, by)
    return lax.dynamic_update_slice(out, block, at)


def take(terms, axis, by, dim):
    at = [jnp.uint32(0)] * terms.ndim
    at[dim] = place_of(axis, by)
    lengths = list(terms.shape)
    lengths[dim] = 1
    return lax.dynamic_slice(terms, at, lengths)


def exchanged(blocks, axis):
    return lax.all_to_all(blocks, axis, 0, 0, tiled=True)


def copies_of_all(block, axis):
    peers = lax.axis_size(axis)
    return exchanged(jnp.broadcast_to(block[None], (peers, *block.shape)), axis)


def gathered_four(block, axis, dim):
    size = lax.axis_size(axis)
    arrived = [shifted(block, axis, k) for k in (1, size - 1, 2)]
    lengths = list(block.shape)
    lengths[dim] = size
    out = jnp.broadcast_to(block, lengths)
    for k, other in zip((1, size - 1, 2), arrived):
        out = put(out, other, axis, -k, dim)
    return out


def sent_four(terms, axis, dim):
    size = lax.axis_size(axis)
    return [take(terms, axis, 0, dim)] + [
        shifted(take(terms, axis, k, dim), axis, k) for k in (1, size - 1, 2)
    ]


def total_of(terms):
    total = terms[0].astype(jnp.float32)
    for other in terms[1:]:
        total = total + other.astype(jnp.float32)
    return total


def added_up(blocks):
    return blocks.astype(jnp.float32).sum(axis=0)


def contract_rows(left, right):
    return lax.dot_general(
        left, right, (((0,), (0,)), ((), ())), preferred_element_type=jnp.float32
    )


def back_kernel(place, gate_t, value_t, value_w, own, *rest):
    others, out, gate_w = rest[:-2], rest[-2], rest[-1]
    groups, share, _ = own.shape
    size = len(others) + 1
    for k, piece in enumerate((own, *others)):
        for group in range(groups):
            start = pl.multiple_of(group * size * share + place[k] * share, share)
            gate_w[pl.ds(start, share), :] = piece[group]
    total = jnp.dot(gate_w[...], gate_t[...], preferred_element_type=jnp.float32)
    total += jnp.dot(value_w[...], value_t[...], preferred_element_type=jnp.float32)
    peers, _, lanes = out.shape
    for peer in range(peers):
        out[peer] = total[:, peer * lanes : (peer + 1) * lanes].astype(out.dtype)


def back_parts(place, gate_t, value_t, value_w, pieces, peers, steps):
    cols, length = gate_t.shape
    width = value_w.shape[0]
    groups, share, _ = pieces[0].shape
    tall = width // steps
    whole = pl.BlockSpec((cols, length), lambda i: (0, 0))
    return pl.pallas_call(
        back_kernel,
        grid=(steps,),
        in_specs=[
            pl.BlockSpec(memory_space=pltpu.SMEM),
            whole,
            whole,
            pl.BlockSpec((tall, cols), lambda i: (i, 0)),
        ]
        + [pl.BlockSpec((groups // steps, share, cols), lambda i: (i, 0, 0))] * len(pieces),
        out_specs=pl.BlockSpec((peers, tall, length // peers), lambda i: (0, i, 0)),
        out_shape=jax.ShapeDtypeStruct((peers, width, length // peers), value_w.dtype),
        scratch_shapes=[pltpu.VMEM((tall, cols), value_w.dtype)],
        compiler_params=pltpu.CompilerParams(
            dimension_semantics=("arbitrary",), vmem_limit_bytes=40 * 2**20
        ),
        cost_estimate=pl.CostEstimate(
            flops=4 * width * cols * length,
            bytes_accessed=4 * (cols * length + width * cols) + 2 * width * length,
            transcendentals=0,
        ),
    )(place, gate_t, value_t, value_w, *pieces)


def on_device(
    tokens, gate_pre, value_pre, up_gate_w, up_value_w, conv_weight, conv_bias, hidden_grad
):
    length, cols = gate_pre.shape
    rows, width = tokens.shape
    nz, nx = lax.axis_size("z"), lax.axis_size("x")
    ny, nc = lax.axis_size("y"), lax.axis_size("c")
    share = up_gate_w.shape[0]
    scale = float(length * nz * nx) ** (-0.5)
    narrow = jnp.bfloat16

    token_blocks = gathered_four(tokens[None], "y", 0)[:, None]
    gate_part = copies_of_all(up_gate_w, "z")
    value_part = gathered_four(up_value_w[None], "x", 0).reshape(nx * share, cols)
    full_value = lax.all_gather(value_part, "z", axis=0, tiled=True)
    steps = (1, nx - 1, 2)
    gate_pieces = [gate_part] + [shifted(gate_part, "x", k) for k in steps]
    gate_places = jnp.stack(
        [(lax.axis_index("x") + nx - k) & (nx - 1) for k in (0, *steps)]
    ).astype(jnp.int32)
    whole_tokens = jnp.broadcast_to(token_blocks, (ny, nc, rows, width))
    other_blocks = swapped(token_blocks, "c", 1)
    whole_tokens = put(whole_tokens, other_blocks, "c", 1, 1)
    whole_tokens = whole_tokens.reshape(length, width)

    gate_pre, value_part = lax.optimization_barrier((gate_pre, value_part))
    gate_float = gate_pre.astype(jnp.float32)
    padded = jnp.pad(gate_float, ((2, 0), (0, 0)))
    gate_conv = (
        conv_bias
        + conv_weight[0] * padded[:length]
        + conv_weight[1] * padded[1 : length + 1]
        + conv_weight[2] * padded[2:]
    )
    active, gelu_back = jax.vjp(jax.nn.gelu, gate_conv)
    grad_float = hidden_grad.astype(jnp.float32)
    value_grad = (grad_float * active).astype(narrow)
    conv_grad = gelu_back(grad_float * value_pre.astype(jnp.float32))[0]
    late = jnp.pad(conv_grad, ((0, 2), (0, 0)))
    gate_grad = (
        conv_weight[2] * conv_grad
        + conv_weight[1] * late[1 : length + 1]
        + conv_weight[0] * late[2:]
    ).astype(narrow)
    conv_terms = jnp.stack(
        [
            jnp.sum(conv_grad * padded[:length], axis=0),
            jnp.sum(conv_grad * padded[1 : length + 1], axis=0),
            jnp.sum(conv_grad * padded[2:], axis=0),
            jnp.sum(conv_grad, axis=0),
        ]
    )
    conv_total = conv_terms
    for axis in ("x", "z"):
        bit = 1
        while bit < lax.axis_size(axis):
            conv_total = conv_total + swapped(conv_total, axis, bit)
            bit *= 2
    conv_total = conv_total * scale

    gate_terms = contract_rows(whole_tokens, gate_grad).astype(narrow)
    value_terms = contract_rows(whole_tokens, value_grad).astype(narrow)
    gate_grad, value_grad, _, _ = lax.optimization_barrier(
        (gate_grad, value_grad, gate_terms, value_terms)
    )
    gate_blocks = sent_four(gate_terms.reshape(nz, nx, share, cols), "x", 1)
    value_sums = lax.psum_scatter(value_terms, "z", scatter_dimension=0, tiled=True)

    part = back_parts(
        gate_places, gate_grad.T, value_grad.T, full_value, gate_pieces, ny * nc, 4
    )
    part = part.reshape(ny, nc, width, rows)
    partner = swapped(take(part, "c", 1, 1), "c", 1)
    pair = total_of([take(part, "c", 0, 1), partner]).astype(narrow)
    input_blocks = sent_four(pair[:, 0], "y", 0)
    input_grad = total_of(input_blocks)[0].astype(narrow)
    input_grad = with_layout_constraint(input_grad, Layout((0, 1))).T

    gate_blocks, _ = lax.optimization_barrier((gate_blocks, pair))
    gate_sums = total_of(gate_blocks).astype(narrow)
    gate_sums = exchanged(gate_sums[:, 0], "z")
    gate_out = added_up(gate_sums) * scale
    value_blocks = sent_four(value_sums.reshape(nx, share, cols), "x", 0)
    value_out = total_of(value_blocks)[0] * scale
    return (input_grad, gate_out, value_out, conv_total[:3], conv_total[3])


def solution(mesh):
    finer = Mesh(mesh.devices.reshape(8, 4, 4, 2), FS_TP)
    in_specs = (
        P(FS_TP, None),
        P(FS, TP),
        P(FS, TP),
        P(FS, TP),
        P(FS, TP),
        P(None, TP),
        P(TP),
        P(FS, TP),
    )
    out_specs = (P(FS_TP, None), P(FS, TP), P(FS, TP), P(None, TP), P(TP))
    return jax.shard_map(
        on_device, mesh=finer, in_specs=in_specs, out_specs=out_specs, check_vma=False
    )
```

```python
import jax
import jax.numpy as jnp
from jax import lax
from jax.experimental import pallas as pl
from jax.experimental.layout import Layout, with_layout_constraint
from jax.experimental.pallas import tpu as pltpu
from jax.sharding import Mesh
from jax.sharding import PartitionSpec as P

FS = ("z", "x")
TP = ("y", "c")
FS_TP = ("z", "x", "y", "c")


def shifted(block, axis, by):
    size = lax.axis_size(axis)
    return lax.ppermute(block, axis, [(i, (i + by) % size) for i in range(size)])


def swapped(block, axis, bit):
    size = lax.axis_size(axis)
    return lax.ppermute(block, axis, [(i, i ^ bit) for i in range(size)])


def place_of(axis, by=0):
    size = lax.axis_size(axis)
    return (lax.axis_index(axis).astype(jnp.uint32) + jnp.uint32(by % size)) & jnp.uint32(size - 1)


def put(out, block, axis, by, dim):
    at = [jnp.uint32(0)] * out.ndim
    at[dim] = place_of(axis, by)
    return lax.dynamic_update_slice(out, block, at)


def take(terms, axis, by, dim):
    at = [jnp.uint32(0)] * terms.ndim
    at[dim] = place_of(axis, by)
    lengths = list(terms.shape)
    lengths[dim] = 1
    return lax.dynamic_slice(terms, at, lengths)


def exchanged(blocks, axis):
    return lax.all_to_all(blocks, axis, 0, 0, tiled=True)


def copies_of_all(block, axis):
    peers = lax.axis_size(axis)
    return exchanged(jnp.broadcast_to(block[None], (peers, *block.shape)), axis)


def gathered_four(block, axis, dim):
    size = lax.axis_size(axis)
    arrived = [shifted(block, axis, k) for k in (1, size - 1, 2)]
    lengths = list(block.shape)
    lengths[dim] = size
    out = jnp.broadcast_to(block, lengths)
    for k, other in zip((1, size - 1, 2), arrived):
        out = put(out, other, axis, -k, dim)
    return out


def sent_four(terms, axis, dim):
    size = lax.axis_size(axis)
    return [take(terms, axis, 0, dim)] + [
        shifted(take(terms, axis, k, dim), axis, k) for k in (1, size - 1, 2)
    ]


def total_of(terms):
    total = terms[0].astype(jnp.float32)
    for other in terms[1:]:
        total = total + other.astype(jnp.float32)
    return total


def added_up(blocks):
    return blocks.astype(jnp.float32).sum(axis=0)


def terms_kernel(place, own, other, gate_t, value_t, gate_out, value_out, tokens):
    groups, rows, _ = own.shape
    for k, piece in enumerate((own, other)):
        for group in range(groups):
            start = pl.multiple_of(group * 2 * rows + place[k] * rows, rows)
            tokens[pl.ds(start, rows), :] = piece[group]
    block = tokens[...]
    value = jnp.dot(value_t[...], block, preferred_element_type=jnp.float32)
    value_out[...] = value.astype(value_out.dtype)
    gate = lax.dot_general(
        block, gate_t[...], (((0,), (1,)), ((), ())), preferred_element_type=jnp.float32
    ).astype(gate_out.dtype)
    peers, tall, share, _ = gate_out.shape
    for far in range(tall):
        for near in range(peers):
            start = (far * peers + near) * share
            gate_out[near, far] = gate[start : start + share]


def grad_terms(place, own, other, gate_t, value_t, far, near, steps):
    groups, rows, width = own.shape
    cols, length = gate_t.shape
    wide, share = width // steps, width // (far * near)
    whole = pl.BlockSpec((cols, length), lambda i: (0, 0))
    piece = pl.BlockSpec((groups, rows, wide), lambda i: (0, 0, i))
    return pl.pallas_call(
        terms_kernel,
        grid=(steps,),
        in_specs=[pl.BlockSpec(memory_space=pltpu.SMEM), piece, piece, whole, whole],
        out_specs=[
            pl.BlockSpec((near, far // steps, share, cols), lambda i: (0, i, 0, 0)),
            pl.BlockSpec((cols, wide), lambda i: (0, i)),
        ],
        out_shape=[
            jax.ShapeDtypeStruct((near, far, share, cols), own.dtype),
            jax.ShapeDtypeStruct((cols, width), own.dtype),
        ],
        scratch_shapes=[pltpu.VMEM((length, wide), own.dtype)],
        compiler_params=pltpu.CompilerParams(
            dimension_semantics=("arbitrary",), vmem_limit_bytes=58 * 2**20
        ),
        cost_estimate=pl.CostEstimate(
            flops=4 * width * cols * length,
            bytes_accessed=4 * (cols * length + width * cols) + 2 * width * length,
            transcendentals=0,
        ),
    )(place, own, other, gate_t, value_t)


def back_kernel(place, gate_t, value_t, value_w, own, *rest):
    others, out, gate_w = rest[:-2], rest[-2], rest[-1]
    groups, share, _ = own.shape
    size = len(others) + 1
    for k, piece in enumerate((own, *others)):
        for group in range(groups):
            start = pl.multiple_of(group * size * share + place[k] * share, share)
            gate_w[pl.ds(start, share), :] = piece[group]
    total = jnp.dot(gate_w[...], gate_t[...], preferred_element_type=jnp.float32)
    total += jnp.dot(value_w[...], value_t[...], preferred_element_type=jnp.float32)
    peers, _, lanes = out.shape
    for peer in range(peers):
        out[peer] = total[:, peer * lanes : (peer + 1) * lanes].astype(out.dtype)


def back_parts(place, gate_t, value_t, value_w, pieces, peers, steps):
    cols, length = gate_t.shape
    width = value_w.shape[0]
    groups, share, _ = pieces[0].shape
    tall = width // steps
    whole = pl.BlockSpec((cols, length), lambda i: (0, 0))
    return pl.pallas_call(
        back_kernel,
        grid=(steps,),
        in_specs=[
            pl.BlockSpec(memory_space=pltpu.SMEM),
            whole,
            whole,
            pl.BlockSpec((tall, cols), lambda i: (i, 0)),
        ]
        + [pl.BlockSpec((groups // steps, share, cols), lambda i: (i, 0, 0))] * len(pieces),
        out_specs=pl.BlockSpec((peers, tall, length // peers), lambda i: (0, i, 0)),
        out_shape=jax.ShapeDtypeStruct((peers, width, length // peers), value_w.dtype),
        scratch_shapes=[pltpu.VMEM((tall, cols), value_w.dtype)],
        compiler_params=pltpu.CompilerParams(
            dimension_semantics=("arbitrary",), vmem_limit_bytes=58 * 2**20
        ),
        cost_estimate=pl.CostEstimate(
            flops=4 * width * cols * length,
            bytes_accessed=4 * (cols * length + width * cols) + 2 * width * length,
            transcendentals=0,
        ),
    )(place, gate_t, value_t, value_w, *pieces)


def on_device(
    tokens, gate_pre, value_pre, up_gate_w, up_value_w, conv_weight, conv_bias, hidden_grad
):
    length, cols = gate_pre.shape
    rows, width = tokens.shape
    nz, nx = lax.axis_size("z"), lax.axis_size("x")
    ny, nc = lax.axis_size("y"), lax.axis_size("c")
    share = up_gate_w.shape[0]
    scale = float(length * nz * nx) ** (-0.5)
    narrow = jnp.bfloat16

    token_blocks = gathered_four(tokens[None], "y", 0)
    other_blocks = swapped(token_blocks, "c", 1)
    core = lax.axis_index("c")
    token_places = jnp.stack([core, nc - 1 - core]).astype(jnp.int32)
    gate_part = copies_of_all(up_gate_w, "z")
    value_part = gathered_four(up_value_w[None], "x", 0).reshape(nx * share, cols)
    full_value = lax.all_gather(value_part, "z", axis=0, tiled=True)
    steps = (1, nx - 1, 2)
    gate_pieces = [gate_part] + [shifted(gate_part, "x", k) for k in steps]
    gate_places = jnp.stack(
        [(lax.axis_index("x") + nx - k) & (nx - 1) for k in (0, *steps)]
    ).astype(jnp.int32)

    gate_pre, value_part = lax.optimization_barrier((gate_pre, value_part))
    gate_float = gate_pre.astype(jnp.float32)
    padded = jnp.pad(gate_float, ((2, 0), (0, 0)))
    gate_conv = (
        conv_bias
        + conv_weight[0] * padded[:length]
        + conv_weight[1] * padded[1 : length + 1]
        + conv_weight[2] * padded[2:]
    )
    active, gelu_back = jax.vjp(jax.nn.gelu, gate_conv)
    grad_float = hidden_grad.astype(jnp.float32)
    value_grad = (grad_float * active).astype(narrow)
    conv_grad = gelu_back(grad_float * value_pre.astype(jnp.float32))[0]
    late = jnp.pad(conv_grad, ((0, 2), (0, 0)))
    gate_grad = (
        conv_weight[2] * conv_grad
        + conv_weight[1] * late[1 : length + 1]
        + conv_weight[0] * late[2:]
    ).astype(narrow)
    conv_terms = jnp.stack(
        [
            jnp.sum(conv_grad * padded[:length], axis=0),
            jnp.sum(conv_grad * padded[1 : length + 1], axis=0),
            jnp.sum(conv_grad * padded[2:], axis=0),
            jnp.sum(conv_grad, axis=0),
        ]
    )
    conv_total = conv_terms
    for axis, bit in (("z", 1), ("z", 2), ("z", 4), ("x", 1), ("x", 2)):
        conv_total = conv_total + swapped(conv_total, axis, bit)
    conv_total = conv_total * scale

    gate_terms, value_terms = grad_terms(
        token_places, token_blocks, other_blocks, gate_grad.T, value_grad.T, nz, nx, 4
    )
    gate_grad, value_grad, _, _ = lax.optimization_barrier(
        (gate_grad, value_grad, gate_terms, value_terms)
    )
    gate_blocks = sent_four(gate_terms, "x", 0)
    value_sums = lax.psum_scatter(value_terms.T, "z", scatter_dimension=0, tiled=True)

    part = back_parts(
        gate_places, gate_grad.T, value_grad.T, full_value, gate_pieces, ny * nc, 4
    )
    part = part.reshape(ny, nc, width, rows)
    partner = swapped(take(part, "c", 1, 1), "c", 1)
    pair = total_of([take(part, "c", 0, 1), partner]).astype(narrow)
    input_blocks = sent_four(pair[:, 0], "y", 0)
    input_grad = total_of(input_blocks)[0].astype(narrow)
    input_grad = with_layout_constraint(input_grad, Layout((0, 1))).T

    gate_blocks, _ = lax.optimization_barrier((gate_blocks, pair))
    gate_sums = total_of(gate_blocks).astype(narrow)
    gate_sums = exchanged(gate_sums[0], "z")
    gate_out = added_up(gate_sums) * scale
    value_blocks = sent_four(value_sums.reshape(nx, share, cols), "x", 0)
    value_out = total_of(value_blocks)[0] * scale
    return (input_grad, gate_out, value_out, conv_total[:3], conv_total[3])


def solution(mesh):
    finer = Mesh(mesh.devices.reshape(8, 4, 4, 2), FS_TP)
    in_specs = (
        P(FS_TP, None),
        P(FS, TP),
        P(FS, TP),
        P(FS, TP),
        P(FS, TP),
        P(None, TP),
        P(TP),
        P(FS, TP),
    )
    out_specs = (P(FS_TP, None), P(FS, TP), P(FS, TP), P(None, TP), P(TP))
    return jax.shard_map(
        on_device, mesh=finer, in_specs=in_specs, out_specs=out_specs, check_vma=False
    )
```

```python
import jax
import jax.numpy as jnp
from jax import lax
from jax.experimental import pallas as pl
from jax.experimental.layout import Layout, with_layout_constraint
from jax.experimental.pallas import tpu as pltpu
from jax.sharding import Mesh
from jax.sharding import PartitionSpec as P

FS = ("z", "x")
TP = ("y", "c")
FS_TP = ("z", "x", "y", "c")


def shifted(block, axis, by):
    size = lax.axis_size(axis)
    return lax.ppermute(block, axis, [(i, (i + by) % size) for i in range(size)])


def swapped(block, axis, bit):
    size = lax.axis_size(axis)
    return lax.ppermute(block, axis, [(i, i ^ bit) for i in range(size)])


def place_of(axis, by=0):
    size = lax.axis_size(axis)
    return (lax.axis_index(axis).astype(jnp.uint32) + jnp.uint32(by % size)) & jnp.uint32(size - 1)


def put(out, block, axis, by, dim):
    at = [jnp.uint32(0)] * out.ndim
    at[dim] = place_of(axis, by)
    return lax.dynamic_update_slice(out, block, at)


def take(terms, axis, by, dim):
    at = [jnp.uint32(0)] * terms.ndim
    at[dim] = place_of(axis, by)
    lengths = list(terms.shape)
    lengths[dim] = 1
    return lax.dynamic_slice(terms, at, lengths)


def exchanged(blocks, axis):
    return lax.all_to_all(blocks, axis, 0, 0, tiled=True)


def copies_of_all(block, axis):
    peers = lax.axis_size(axis)
    return exchanged(jnp.broadcast_to(block[None], (peers, *block.shape)), axis)


def gathered_four(block, axis, dim):
    size = lax.axis_size(axis)
    arrived = [shifted(block, axis, k) for k in (1, size - 1, 2)]
    lengths = list(block.shape)
    lengths[dim] = size
    out = jnp.broadcast_to(block, lengths)
    for k, other in zip((1, size - 1, 2), arrived):
        out = put(out, other, axis, -k, dim)
    return out


def sent_four(terms, axis, dim):
    size = lax.axis_size(axis)
    return [take(terms, axis, 0, dim)] + [
        shifted(take(terms, axis, k, dim), axis, k) for k in (1, size - 1, 2)
    ]


def total_of(terms):
    total = terms[0].astype(jnp.float32)
    for other in terms[1:]:
        total = total + other.astype(jnp.float32)
    return total


def added_up(blocks):
    return blocks.astype(jnp.float32).sum(axis=0)


def terms_kernel(place, gate_t, value_t, *rest):
    pieces, gate_out, value_out, tokens = rest[:-3], rest[-3], rest[-2], rest[-1]
    for k, piece in enumerate(pieces):
        rows = piece.shape[0]
        start = pl.multiple_of(place[k] * rows, rows)
        tokens[pl.ds(start, rows), :] = piece[...]
    block = tokens[...]
    value = jnp.dot(value_t[...], block, preferred_element_type=jnp.float32)
    value_out[...] = value.astype(value_out.dtype)
    gate = lax.dot_general(
        block, gate_t[...], (((0,), (1,)), ((), ())), preferred_element_type=jnp.float32
    ).astype(gate_out.dtype)
    peers, tall, share, _ = gate_out.shape
    for far in range(tall):
        for near in range(peers):
            start = (far * peers + near) * share
            gate_out[near, far] = gate[start : start + share]


def grad_terms(place, pieces, gate_t, value_t, far, near, steps):
    rows, width = pieces[0].shape
    kind = pieces[0].dtype
    cols, length = gate_t.shape
    wide, share = width // steps, width // (far * near)
    whole = pl.BlockSpec((cols, length), lambda i: (0, 0))
    piece = pl.BlockSpec((rows, wide), lambda i: (0, i))
    return pl.pallas_call(
        terms_kernel,
        grid=(steps,),
        in_specs=[pl.BlockSpec(memory_space=pltpu.SMEM), whole, whole] + [piece] * len(pieces),
        out_specs=[
            pl.BlockSpec((near, far // steps, share, cols), lambda i: (0, i, 0, 0)),
            pl.BlockSpec((cols, wide), lambda i: (0, i)),
        ],
        out_shape=[
            jax.ShapeDtypeStruct((near, far, share, cols), kind),
            jax.ShapeDtypeStruct((cols, width), kind),
        ],
        scratch_shapes=[pltpu.VMEM((length, wide), kind)],
        compiler_params=pltpu.CompilerParams(
            dimension_semantics=("arbitrary",), vmem_limit_bytes=58 * 2**20
        ),
        cost_estimate=pl.CostEstimate(
            flops=4 * width * cols * length,
            bytes_accessed=4 * (cols * length + width * cols) + 2 * width * length,
            transcendentals=0,
        ),
    )(place, gate_t, value_t, *pieces)


def back_kernel(place, gate_t, value_t, value_w, own, *rest):
    others, out, gate_w = rest[:-2], rest[-2], rest[-1]
    groups, share, _ = own.shape
    size = len(others) + 1
    for k, piece in enumerate((own, *others)):
        for group in range(groups):
            start = pl.multiple_of(group * size * share + place[k] * share, share)
            gate_w[pl.ds(start, share), :] = piece[group]
    total = jnp.dot(gate_w[...], gate_t[...], preferred_element_type=jnp.float32)
    total += jnp.dot(value_w[...], value_t[...], preferred_element_type=jnp.float32)
    peers, _, lanes = out.shape
    for peer in range(peers):
        out[peer] = total[:, peer * lanes : (peer + 1) * lanes].astype(out.dtype)


def back_parts(place, gate_t, value_t, value_w, pieces, peers, steps):
    cols, length = gate_t.shape
    width = value_w.shape[0]
    groups, share, _ = pieces[0].shape
    tall = width // steps
    whole = pl.BlockSpec((cols, length), lambda i: (0, 0))
    return pl.pallas_call(
        back_kernel,
        grid=(steps,),
        in_specs=[
            pl.BlockSpec(memory_space=pltpu.SMEM),
            whole,
            whole,
            pl.BlockSpec((tall, cols), lambda i: (i, 0)),
        ]
        + [pl.BlockSpec((groups // steps, share, cols), lambda i: (i, 0, 0))] * len(pieces),
        out_specs=pl.BlockSpec((peers, tall, length // peers), lambda i: (0, i, 0)),
        out_shape=jax.ShapeDtypeStruct((peers, width, length // peers), value_w.dtype),
        scratch_shapes=[pltpu.VMEM((tall, cols), value_w.dtype)],
        compiler_params=pltpu.CompilerParams(
            dimension_semantics=("arbitrary",), vmem_limit_bytes=58 * 2**20
        ),
        cost_estimate=pl.CostEstimate(
            flops=4 * width * cols * length,
            bytes_accessed=4 * (cols * length + width * cols) + 2 * width * length,
            transcendentals=0,
        ),
    )(place, gate_t, value_t, value_w, *pieces)


def on_device(
    tokens, gate_pre, value_pre, up_gate_w, up_value_w, conv_weight, conv_bias, hidden_grad
):
    length, cols = gate_pre.shape
    rows, width = tokens.shape
    nz, nx = lax.axis_size("z"), lax.axis_size("x")
    ny, nc = lax.axis_size("y"), lax.axis_size("c")
    share = up_gate_w.shape[0]
    scale = float(length * nz * nx) ** (-0.5)
    narrow = jnp.bfloat16

    steps = (1, nx - 1, 2)
    pieces = [tokens] + [shifted(tokens, "y", k) for k in steps]
    pieces = pieces + [swapped(piece, "c", 1) for piece in pieces]
    core = lax.axis_index("c")
    chips = [(lax.axis_index("y") + ny - k) & (ny - 1) for k in (0, *steps)]
    token_places = jnp.stack(
        [chip * nc + core for chip in chips] + [chip * nc + nc - 1 - core for chip in chips]
    ).astype(jnp.int32)
    gate_part = copies_of_all(up_gate_w, "z")
    value_part = gathered_four(up_value_w[None], "x", 0).reshape(nx * share, cols)
    full_value = lax.all_gather(value_part, "z", axis=0, tiled=True)
    gate_pieces = [gate_part] + [shifted(gate_part, "x", k) for k in steps]
    gate_places = jnp.stack(
        [(lax.axis_index("x") + nx - k) & (nx - 1) for k in (0, *steps)]
    ).astype(jnp.int32)

    gate_pre, value_part = lax.optimization_barrier((gate_pre, value_part))
    gate_float = gate_pre.astype(jnp.float32)
    padded = jnp.pad(gate_float, ((2, 0), (0, 0)))
    gate_conv = (
        conv_bias
        + conv_weight[0] * padded[:length]
        + conv_weight[1] * padded[1 : length + 1]
        + conv_weight[2] * padded[2:]
    )
    active, gelu_back = jax.vjp(jax.nn.gelu, gate_conv)
    grad_float = hidden_grad.astype(jnp.float32)
    value_grad = (grad_float * active).astype(narrow)
    conv_grad = gelu_back(grad_float * value_pre.astype(jnp.float32))[0]
    late = jnp.pad(conv_grad, ((0, 2), (0, 0)))
    gate_grad = (
        conv_weight[2] * conv_grad
        + conv_weight[1] * late[1 : length + 1]
        + conv_weight[0] * late[2:]
    ).astype(narrow)
    conv_terms = jnp.stack(
        [
            jnp.sum(conv_grad * padded[:length], axis=0),
            jnp.sum(conv_grad * padded[1 : length + 1], axis=0),
            jnp.sum(conv_grad * padded[2:], axis=0),
            jnp.sum(conv_grad, axis=0),
        ]
    )
    conv_total = conv_terms
    for axis, bit in (("z", 1), ("z", 2), ("z", 4), ("x", 1), ("x", 2)):
        conv_total = conv_total + swapped(conv_total, axis, bit)
    conv_total = conv_total * scale

    gate_t, value_t = gate_grad.T, value_grad.T
    gate_terms, value_terms = grad_terms(
        token_places, pieces, gate_t, value_t, nz, nx, 4
    )
    gate_blocks = sent_four(gate_terms, "x", 0)
    value_sums = lax.psum_scatter(value_terms.T, "z", scatter_dimension=0, tiled=True)

    part = back_parts(
        gate_places, gate_t, value_t, full_value, gate_pieces, ny * nc, 4
    )
    part = part.reshape(ny, nc, width, rows)
    partner = swapped(take(part, "c", 1, 1), "c", 1)
    pair = total_of([take(part, "c", 0, 1), partner]).astype(narrow)
    input_blocks = sent_four(pair[:, 0], "y", 0)
    input_grad = total_of(input_blocks)[0].astype(narrow)
    input_grad = with_layout_constraint(input_grad, Layout((0, 1))).T

    gate_blocks, _ = lax.optimization_barrier((gate_blocks, pair))
    gate_sums = total_of(gate_blocks).astype(narrow)
    gate_sums = exchanged(gate_sums[0], "z")
    gate_out = added_up(gate_sums) * scale
    value_blocks = sent_four(value_sums.reshape(nx, share, cols), "x", 0)
    value_out = total_of(value_blocks)[0] * scale
    return (input_grad, gate_out, value_out, conv_total[:3], conv_total[3])


def solution(mesh):
    finer = Mesh(mesh.devices.reshape(8, 4, 4, 2), FS_TP)
    in_specs = (
        P(FS_TP, None),
        P(FS, TP),
        P(FS, TP),
        P(FS, TP),
        P(FS, TP),
        P(None, TP),
        P(TP),
        P(FS, TP),
    )
    out_specs = (P(FS_TP, None), P(FS, TP), P(FS, TP), P(None, TP), P(TP))
    return jax.shard_map(
        on_device, mesh=finer, in_specs=in_specs, out_specs=out_specs, check_vma=False
    )
```
